32 devices in a mesh: grp: 2 (over y), ep: 4 (over z), tp: 4 (over x, core).
Axes of the slice: x: 2, y: 2, z: 4, core: 2. Of those that a mesh axis runs over, the one named last changes fastest.
Arguments:
- mix_input: bfloat16 [2048, 2048], P(('grp', 'ep'), 'tp'), parts along dimension 0, may hold values from -6 to 6
- group_weight: bfloat16 [16, 128, 128], replicated, may hold values from -0.5 to 0.5
- pool_gain: float32 [2048], replicated, may hold values from 0.1 to 1.9
- branch_weight: bfloat16 [2048, 2048], P('tp'), may hold values from -0.125 to 0.125
- exp_input: bfloat16 [1024, 2048], P(('grp', 'ep')), parts along dimension 0, may hold values from -6 to 6
- norm_gain: float32 [2048], replicated, may hold values from 0.1 to 1.9
- routes: int32 [1024, 2], P(('grp', 'ep')), parts along dimension 0, may hold values from 0 to 3, all different within a row; in each aligned block of 128 rows (0 to 127, 128 to 255, ...) at most 96 rows name the same one
- route_weights: float32 [1024, 2], P(('grp', 'ep')), parts along dimension 0, may hold values from 0.25 to 1
- gate_weight: bfloat16 [4, 2048, 3584], P('ep', None, 'tp'), may hold values from -0.125 to 0.125
- up_weight: bfloat16 [4, 2048, 3584], P('ep', None, 'tp'), may hold values from -0.125 to 0.125
- down_weight: bfloat16 [4, 3584, 2048], P('ep', 'tp'), may hold values from -0.09375 to 0.09375
Outputs:
- mix_out: bfloat16 [2048, 2048], P(('grp', 'ep'), 'tp'), parts along dimension 0
- exp_out: bfloat16 [1024, 2048], P(('grp', 'ep'), 'tp'), parts along dimension 0
The draws below stay inside these ranges and needn't reach their ends.
There are 2 independent parts, one for each index of `grp`. The reference program is written for one: setup_inputs(seed, part) draws one part's arguments, and reference() takes and returns one part's arrays. A program takes and returns all parts, laid end to end along the dimension named above; an argument that names none is the same for every part. Nothing has to cross between parts.
Inputs may be any that keep to these rules, and one draw needn't show every extreme that they name: `routes`: the 2 experts of a token differ. Among the 128 tokens of one index of ep no expert is named by more than 96 of them, a bound that some block reaches.
All inputs are finite; a program needn't handle non-finite values.
Results may differ from the reference program's by a relative error of at most 0.018.
Values may be sent and summed in bfloat16 or wider, within the bound.
A program may use at most 64 MiB of HBM per device.

```python
import math
import jax
import jax.numpy as jnp
import numpy as np
from jax import lax

WIDTH = 2048
GROUPS = 16
GROUP_WIDTH = 128
HIDDEN_SIZE = 3584
TOP_K = 2
TOK_EXP = 128
POOL_WIDTH = 2048
EXPERTS = 4
MIX_TOKENS = 1024
EXP_TOKENS = 512
EXP_ROWS = 384
CAP_SLOTS = 96
N_TP = 4


def steps_of(rng, dims, shards, smallest, largest):
    loudness, own = 1.0, jax.random.fold_in(rng, 6)
    for position, shards_of in shards:
        steps = jnp.exp(jax.random.uniform(jax.random.fold_in(own, position), (shards_of,), jnp.float32, smallest / len(shards), largest / len(shards)))
        loudness = loudness * jnp.repeat(steps, dims[position] // shards_of).reshape([-1 if axis == position else 1 for axis in range(len(dims))])
    return loudness


def assign_block(rng, own, number, rows, count, top, bound, slope):
    order = jax.random.permutation(rng, count)
    heavy_load, ordinary = load_shares(count, rows * top, bound, slope, True), load_shares(count, rows * top, bound, slope, False)
    places = jnp.arange(count)

    def named(sizes, offset_by):
        used = int((sizes > 0).sum())
        fixed = max(1, used // 4)
        passed = fixed + (places - fixed + offset_by * (used - fixed)) % max(1, count - fixed)
        return jnp.zeros((count,), jnp.int32).at[order[jnp.where(places < fixed, places, passed)]].set(jnp.asarray(sizes, jnp.int32))

    sizes = jnp.where(number % 4 == 0, named(heavy_load, number // 4), named(ordinary, number - number // 4 - 1))
    mixed = jax.random.permutation(jax.random.fold_in(own, 3), count)
    giver, sink = mixed[0:count // 2 * 2:2], mixed[1:count // 2 * 2:2]
    room = jnp.minimum(sizes[giver] - 1, bound - sizes[sink]) // 2
    room = jnp.where((giver == order[0]) | (sink == order[0]) | (sizes[sink] == 0), 0, jnp.maximum(room, 0))
    passed = jax.random.randint(jax.random.fold_in(own, 4), (count // 2,), 0, 1 << 20) % (room + 1)
    sizes = sizes.at[giver].add(-passed).at[sink].add(passed)
    labels = jnp.searchsorted(jnp.cumsum(sizes), jnp.arange(rows * top), side="right").astype(jnp.int32)
    grid = labels.reshape(top, rows).T
    grid = grid[jax.random.permutation(jax.random.fold_in(own, 1), rows)]
    offset_by = jax.random.randint(jax.random.fold_in(own, 2), (rows, 1), 0, top)
    return jnp.take_along_axis(grid, (jnp.arange(top)[None, :] + offset_by) % top, axis=1)


def load_shares(count, total, limit, skew, full):
    weights = [(1 << 20) // math.isqrt(standing ** skew) + 1 for standing in range(1, count + 1)]
    largest = limit if full else min(limit, max(-(-total // count), total * weights[0] // sum(weights)))
    least = 1 if total - largest >= count - 1 else 0
    given, spare = [largest] + [least] * (count - 1), total - largest - least * (count - 1)
    while spare > 0:
        free = [i for i in range(1, count) if given[i] < largest] or [i for i in range(1, count) if given[i] < limit]
        mass, budget = sum([weights[i] for i in free]), spare
        for i in free:
            more = min(limit - given[i], max(1, budget * weights[i] // mass), spare)
            given[i] = given[i] + more
            spare = spare - more
    return np.array(given)


def gaussian(rng, shape, spread, bound, split=(), kind=jnp.bfloat16):
    drawn = spread * jax.random.normal(rng, shape, jnp.float32)
    if split:
        drawn = drawn * steps_of(rng, shape, split, -0.22, 0.18)
    return jnp.clip(drawn, -bound, bound).astype(kind)


def setup_inputs(seed: int = 0, part: int = 0) -> dict:
    key_list = jax.random.split(jax.random.key(seed), 12)
    own_keys = jax.random.split(jax.random.fold_in(key_list[11], part), 12)
    mix_input = gaussian(own_keys[0], (MIX_TOKENS, POOL_WIDTH), 1.0, 6.0, ((0, 4), (1, 4)))
    group_weight = gaussian(key_list[1], (GROUPS, GROUP_WIDTH, GROUP_WIDTH), GROUP_WIDTH ** -0.5, 0.5)
    pool_gain = jnp.clip(1.0 + 0.18 * jax.random.normal(key_list[2], (POOL_WIDTH,), jnp.float32), 0.1, 1.9)
    branch_weight = gaussian(key_list[3], (POOL_WIDTH, WIDTH), POOL_WIDTH ** -0.5, 0.125, ((0, 4),))
    exp_input = gaussian(own_keys[4], (EXP_TOKENS, WIDTH), 1.0, 6.0, ((0, 4),))
    norm_gain = jnp.clip(1.0 + 0.18 * jax.random.normal(key_list[5], (WIDTH,), jnp.float32), 0.1, 1.9)
    routes_keys = jax.random.split(jax.random.fold_in(own_keys[6], 1), EXP_TOKENS // TOK_EXP)
    routes_turns = jax.random.permutation(jax.random.fold_in(own_keys[6], 3), EXP_TOKENS // TOK_EXP)
    routes = jax.vmap(lambda own, number: assign_block(jax.random.fold_in(own_keys[6], 2), own, number, TOK_EXP, EXPERTS, TOP_K, CAP_SLOTS, 1))(routes_keys, routes_turns).reshape((EXP_TOKENS, TOP_K))
    route_weights = jnp.clip(0.25 + 0.75 * jax.random.uniform(own_keys[7], (EXP_TOKENS, TOP_K), jnp.float32) ** steps_of(own_keys[7], (EXP_TOKENS, TOP_K), ((0, 4),), -0.2, 0.2), 0.25, 1.0)
    gate_weight = gaussian(key_list[8], (EXPERTS, WIDTH, HIDDEN_SIZE), WIDTH ** -0.5, 0.125, ((0, 4), (2, 4)))
    up_weight = gaussian(key_list[9], (EXPERTS, WIDTH, HIDDEN_SIZE), WIDTH ** -0.5, 0.125, ((0, 4), (2, 4)))
    down_weight = gaussian(key_list[10], (EXPERTS, HIDDEN_SIZE, WIDTH), HIDDEN_SIZE ** -0.5, 0.09375, ((0, 4), (1, 4)))
    return dict(mix_input=mix_input, group_weight=group_weight, pool_gain=pool_gain, branch_weight=branch_weight, exp_input=exp_input, norm_gain=norm_gain, routes=routes, route_weights=route_weights, gate_weight=gate_weight, up_weight=up_weight, down_weight=down_weight)


windows = (2, 4, 8, 16)
epsilon = 1e-06

def trailing_sums(extended, rows):
    span_two = extended[1:] + extended[:-1]
    span_four = span_two[2:] + span_two[:-2]
    span_eight = span_four[4:] + span_four[:-4]
    span_sixteen = span_eight[8:] + span_eight[:-8]
    return [span_two[-rows:], span_four[-rows:], span_eight[-rows:], span_sixteen[-rows:]]

def pooled_deviation(extended, positions, group_ids, group_width, rows):
    sums = trailing_sums(extended, rows)
    current = extended[-rows:]
    window_id = jnp.repeat(group_ids % 4, group_width)
    result = jnp.zeros_like(current)
    for window_level, window_len in enumerate(windows):
        counted = jnp.minimum(positions + 1, window_len).astype(jnp.float32)[:, None]
        result = jnp.where(window_id[None, :] == window_level, sums[window_level] / counted - current, result)
    return result

def blockwise_product(left, right, blocks):
    inner = left.shape[1] // blocks
    left_pieces = left.reshape(left.shape[0], blocks, inner).transpose(1, 0, 2)
    right_pieces = right.reshape(blocks, inner, right.shape[1])

    def add_block(running, operands):
        piece, weight = operands
        rounded = lax.optimization_barrier(jnp.dot(piece, weight, preferred_element_type=jnp.float32).astype(jnp.bfloat16))
        return (running + rounded.astype(jnp.float32), None)
    start_sum = jnp.zeros((left.shape[0], right.shape[1]), jnp.float32)
    running, _ = lax.scan(add_block, start_sum, (left_pieces, right_pieces))
    return running.astype(jnp.bfloat16)

def reference(mix_input, group_weight, pool_gain, branch_weight, exp_input, norm_gain, routes, route_weights, gate_weight, up_weight, down_weight):
    rows = mix_input.shape[0]
    extended = jnp.concatenate([jnp.zeros((15, POOL_WIDTH), jnp.float32), mix_input.astype(jnp.float32)], axis=0)
    positions = jnp.arange(rows, dtype=jnp.int32)
    group_ids = jnp.arange(GROUPS, dtype=jnp.int32)
    deviation = pooled_deviation(extended, positions, group_ids, GROUP_WIDTH, rows).astype(jnp.bfloat16)
    grouped = jnp.einsum('rgc,gcd->rgd', deviation.reshape(rows, GROUPS, GROUP_WIDTH).astype(jnp.float32), group_weight.astype(jnp.float32)).reshape(rows, POOL_WIDTH)
    pooled = (grouped * pool_gain).astype(jnp.bfloat16)
    mix_out = blockwise_product(pooled, branch_weight, N_TP)
    tokens = exp_input.shape[0]
    floated = exp_input.astype(jnp.float32)
    normed = (floated * lax.rsqrt(lax.optimization_barrier(jnp.mean(floated * floated, axis=1, keepdims=True)) + epsilon) * norm_gain).astype(jnp.bfloat16)
    flat_expert = routes.reshape(-1).astype(jnp.int32)
    assignments = flat_expert.shape[0]
    onehot = (flat_expert[:, None] == jnp.arange(EXPERTS, dtype=jnp.int32)[None, :]).astype(jnp.int32)
    slot_rank = lax.optimization_barrier(jnp.sum((jnp.cumsum(onehot, axis=0) - onehot) * onehot, axis=1)).astype(jnp.int32)
    token_of = (jnp.arange(assignments, dtype=jnp.int32) // TOP_K).astype(jnp.int32)
    slot_table = jnp.full((EXPERTS, EXP_ROWS), tokens, jnp.int32).at[flat_expert, slot_rank].set(token_of)
    padded = jnp.concatenate([normed, jnp.zeros((1, WIDTH), jnp.bfloat16)], axis=0)

    def one_expert(operands):
        row_index, w_gate, w_up, w_down = operands
        chosen = padded[row_index]
        gate_pre = jnp.dot(chosen, w_gate, preferred_element_type=jnp.float32)
        up_pre = jnp.dot(chosen, w_up, preferred_element_type=jnp.float32)
        hidden = (jax.nn.silu(gate_pre) * up_pre).astype(jnp.bfloat16)
        return blockwise_product(hidden, w_down, N_TP)
    outputs = lax.map(one_expert, (slot_table, gate_weight, up_weight, down_weight))
    picked = outputs[flat_expert, slot_rank].astype(jnp.float32).reshape(tokens, TOP_K, WIDTH)
    exp_out = lax.optimization_barrier(jnp.sum(picked * route_weights[:, :, None], axis=1)).astype(jnp.bfloat16)
    return (mix_out, exp_out)
```

```python
import functools

import jax
import jax.numpy as jnp
from jax import lax
from jax.experimental import pallas as pl
from jax.experimental.pallas import tpu as pltpu
from jax.sharding import PartitionSpec as P

windows = (2, 4, 8, 16)
epsilon = 1e-06


def shifted(block, axis, distance):
    devices = range(lax.axis_size(axis))
    route = [(i - distance, i) for i in devices if i - distance in devices]
    return lax.ppermute(block, axis, route)


def trailing_sums(extended, rows):
    span_two = extended[1:] + extended[:-1]
    span_four = span_two[2:] + span_two[:-2]
    span_eight = span_four[4:] + span_four[:-4]
    span_sixteen = span_eight[8:] + span_eight[:-8]
    return [span_two[-rows:], span_four[-rows:], span_eight[-rows:], span_sixteen]


def pooled_deviation(extended, positions, group_ids, group_width, rows):
    sums = trailing_sums(extended, rows)
    current = extended[-rows:]
    window_id = jnp.repeat(group_ids % 4, group_width)
    result = jnp.zeros_like(current)
    for window_level, window_len in enumerate(windows):
        counted = jnp.minimum(positions + 1, window_len).astype(jnp.float32)[:, None]
        result = jnp.where(
            window_id[None, :] == window_level, sums[window_level] / counted - current, result
        )
    return result


def on_device(
    mix_input,
    group_weight,
    pool_gain,
    branch_weight,
    exp_input,
    norm_gain,
    routes,
    route_weights,
    gate_weight,
    up_weight,
    down_weight,
):
    tp_rank = lax.axis_index("tp")
    ep_rank = lax.axis_index("ep")
    rows_mix, channels = mix_input.shape
    group_width = group_weight.shape[1]
    group_count = channels // group_width
    first_group = tp_rank * group_count
    last_rows = mix_input[rows_mix - 15 :]
    before = shifted(last_rows, "ep", 1)
    extended = jnp.concatenate([before, mix_input], axis=0).astype(jnp.float32)
    positions = ep_rank * rows_mix + jnp.arange(rows_mix, dtype=jnp.int32)
    group_ids = first_group + jnp.arange(group_count, dtype=jnp.int32)
    deviation = pooled_deviation(extended, positions, group_ids, group_width, rows_mix).astype(
        jnp.bfloat16
    )
    own_groups = lax.dynamic_slice_in_dim(group_weight, first_group, group_count, 0)
    grouped = jnp.einsum(
        "rgc,gcd->rgd",
        deviation.reshape(rows_mix, group_count, group_width),
        own_groups,
        preferred_element_type=jnp.float32,
    ).reshape(rows_mix, channels)
    own_gain = lax.dynamic_slice_in_dim(pool_gain, first_group * group_width, channels, 0)
    pooled = (grouped * own_gain).astype(jnp.bfloat16)
    tok_rows, width = exp_input.shape
    columns = width // lax.axis_size("tp")
    experts_all = lax.axis_size("ep")
    capacity = 3 * tok_rows // experts_all
    floated = exp_input.astype(jnp.float32)
    normed = (
        floated
        * lax.rsqrt(jnp.mean(floated * floated, axis=1, keepdims=True) + epsilon)
        * norm_gain
    ).astype(jnp.bfloat16)
    flat_expert = routes.reshape(-1)
    assignments = flat_expert.shape[0]
    onehot = (flat_expert[:, None] == jnp.arange(experts_all, dtype=jnp.int32)[None, :]).astype(
        jnp.int32
    )
    slot_rank = jnp.sum((jnp.cumsum(onehot, axis=0) - onehot) * onehot, axis=1)
    slot_index = flat_expert * capacity + slot_rank
    token_of = jnp.arange(assignments, dtype=jnp.int32) // routes.shape[1]
    slot_token = (
        jnp.full((experts_all * capacity,), tok_rows, jnp.int32).at[slot_index].set(token_of)
    )
    padded = jnp.concatenate([normed, jnp.zeros((1, width), jnp.bfloat16)], axis=0)
    w_gate = gate_weight[0]
    w_up = up_weight[0]
    w_down = down_weight[0]
    arrived_rows = experts_all * capacity
    own_columns = lax.dynamic_slice_in_dim(padded, tp_rank * columns, columns, 1)
    outgoing = own_columns[slot_token].reshape(experts_all, capacity, columns)
    arrived = lax.all_to_all(outgoing, "ep", split_axis=0, concat_axis=0, tiled=True).reshape(
        arrived_rows, columns
    )
    section = lax.all_gather(arrived, "tp", axis=1, tiled=True)
    gate_pre = jnp.dot(section, w_gate, preferred_element_type=jnp.float32)
    up_pre = jnp.dot(section, w_up, preferred_element_type=jnp.float32)
    hidden = (jax.nn.silu(gate_pre) * up_pre).astype(jnp.bfloat16)
    weight_cols = branch_weight
    mix_sum = lax.psum_scatter(
        lax.dot_general(
            weight_cols, pooled, (((0,), (1,)), ((), ())), preferred_element_type=jnp.float32
        ).astype(jnp.bfloat16),
        "tp",
        scatter_dimension=0,
        tiled=True,
    )
    weight_cols = w_down
    exp_sum = lax.psum_scatter(
        lax.dot_general(
            weight_cols, hidden, (((0,), (1,)), ((), ())), preferred_element_type=jnp.float32
        ).astype(jnp.bfloat16),
        "tp",
        scatter_dimension=0,
        tiled=True,
    )
    mix_out = mix_sum.T
    results = exp_sum.reshape(columns, experts_all, capacity)
    returned = lax.all_to_all(results, "ep", split_axis=1, concat_axis=1, tiled=True).reshape(
        columns, experts_all * capacity
    )
    picked = returned[:, slot_index].astype(jnp.float32)
    weighted = picked * route_weights.reshape(-1)[None, :]
    combined = jnp.sum(weighted.reshape(columns, tok_rows, routes.shape[1]), axis=2)
    exp_out = combined.T.astype(jnp.bfloat16)
    return (mix_out, exp_out)


lanes = 128
MESH = pl.DeviceIdType.MESH
f32 = jnp.float32
bf16 = jnp.bfloat16


def fused_kernel(
    x_ref,
    norm_ref,
    routes_ref,
    weights_ref,
    mix_ref,
    gain_ref,
    groups_hbm,
    branch_hbm,
    gate_hbm,
    up_hbm,
    down_hbm,
    mix_out,
    exp_out,
    wgu,
    wd,
    wb,
    gw,
    xn,
    sb,
    xg,
    gu,
    hid,
    halo,
    pooled,
    keep_m,
    ps_m,
    pr_m,
    xs_m,
    xr_m,
    keep,
    ps,
    pr,
    xs,
    xr,
    zs,
    zr,
    w_sem,
    d_send,
    d_recv,
    r_send,
    r_recv,
    z_send,
    z_recv,
    m_send,
    m_recv,
    h_sem,
):
    z = lax.axis_index("ep")
    t = lax.axis_index("tp")
    near = t + 1 - 2 * (t % 2)
    across = (t + 2) % 4
    diagonal = (near + 2) % 4
    peers = [z, z + 1 - 2 * (z % 2), 3 - z, (z + 2) % 4]
    tokens, width = x_ref.shape
    quarter = width // 4
    cap = xg.shape[2]
    hid_tiles = gate_hbm.shape[2] // lanes
    rows_mix, channels = mix_ref.shape
    group_count = channels // lanes

    loads = []
    for i in range(2 * hid_tiles):
        src = gate_hbm if i < hid_tiles else up_hbm
        at = (i % hid_tiles) * lanes
        loads.append(
            pltpu.make_async_copy(
                src.at[0, :, pl.ds(at, lanes)],
                wgu.at[i // 2, :, pl.ds((i % 2) * lanes, lanes)],
                w_sem.at[i],
            )
        )
    n0 = 2 * hid_tiles
    load_b = [
        pltpu.make_async_copy(branch_hbm.at[:, pl.ds(k * quarter, quarter)], wb.at[k], w_sem.at[n0 + k])
        for k in range(4)
    ]
    load_d = [
        pltpu.make_async_copy(down_hbm.at[0, :, pl.ds(k * quarter, quarter)], wd.at[k], w_sem.at[n0 + 4 + k])
        for k in range(4)
    ]
    load_g = pltpu.make_async_copy(groups_hbm.at[pl.ds(t * group_count, group_count)], gw, w_sem.at[n0 + 8])
    load_g.start()
    for c in load_b + loads + load_d:
        c.start()

    barrier = pltpu.get_barrier_semaphore()
    for k in (1, 2, 3):
        pl.semaphore_signal(barrier, inc=1, device_id={"ep": peers[k]}, device_id_type=MESH)
    for k in (near, across):
        pl.semaphore_signal(barrier, inc=1, device_id={"tp": k}, device_id_type=MESH)

    def remote(src, dst, send, recv, who):
        return pltpu.make_async_remote_copy(
            src_ref=src, dst_ref=dst, send_sem=send, recv_sem=recv, device_id=who, device_id_type=MESH
        )

    floated = x_ref[...].astype(f32)
    scale = lax.rsqrt(jnp.mean(floated * floated, axis=1, keepdims=True) + epsilon)
    xn_val = (floated * scale * norm_ref[...]).astype(bf16)
    for k in range(4):
        xn[k] = xn_val[:, k * quarter : (k + 1) * quarter]
    r0 = routes_ref[:, 0:1]
    r1 = routes_ref[:, 1:2]
    lane = lax.broadcasted_iota(jnp.int32, (tokens, lanes), 1)
    member = ((r0 == lane) | (r1 == lane)).astype(f32)
    above = (
        lax.broadcasted_iota(jnp.int32, (tokens, tokens), 0)
        > lax.broadcasted_iota(jnp.int32, (tokens, tokens), 1)
    ).astype(f32)
    rank = jnp.dot(above.astype(bf16), member.astype(bf16), preferred_element_type=f32)
    slot_lane = lax.broadcasted_iota(jnp.int32, (tokens, cap), 1)
    places = []
    shares = []
    for k in range(4):
        own = jnp.sum(jnp.where(lane == peers[k], rank, 0.0), axis=1, keepdims=True).astype(jnp.int32)
        named = (r0 == peers[k]) | (r1 == peers[k])
        slot = jnp.where(named, own, cap)
        places.append((slot_lane == slot).astype(f32).astype(bf16))
        shares.append(
            jnp.where(r0 == peers[k], weights_ref[:, 0:1], 0.0)
            + jnp.where(r1 == peers[k], weights_ref[:, 1:2], 0.0)
        )

    def gathered(k, block):
        return lax.dot_general(
            places[k], block, (((0,), (0,)), ((), ())), preferred_element_type=f32
        ).astype(bf16)

    own_cols = xn[t]
    for k in (1, 2, 3):
        sb[k] = gathered(k, own_cols)
    pl.semaphore_wait(barrier, 5)
    d_z = []
    for k in (1, 2, 3):
        c = remote(sb.at[k], xg.at[t, k], d_send.at[k - 1, 0], d_recv.at[k - 1, 0], {"ep": peers[k]})
        c.start()
        d_z.append(c)
    halo_copy = remote(
        mix_ref.at[pl.ds(rows_mix - 16, 16), :], halo, h_sem.at[0], h_sem.at[1], {"ep": (z + 1) % 4}
    )

    @pl.when(z < 3)
    def _():
        halo_copy.start()

    for q in range(4):
        xg[q, 0] = gathered(0, xn[q])

    @pl.when(z == 0)
    def _():
        halo[...] = jnp.zeros_like(halo)

    @pl.when(z > 0)
    def _():
        halo_copy.wait_recv()

    load_g.wait()
    position = z * rows_mix + lax.broadcasted_iota(jnp.int32, (rows_mix, lanes), 0)
    for g in range(group_count):
        cols = slice(g * lanes, (g + 1) * lanes)
        current = mix_ref[:, cols].astype(f32)
        total = jnp.concatenate([halo[:, cols].astype(f32), current], axis=0)
        level = g % 4
        for step in range(level + 1):
            total = total + pltpu.roll(total, 1 << step, 0)
        counted = jnp.minimum(position + 1, windows[level]).astype(f32)
        deviation = (total[16:] / counted - current).astype(bf16)
        grouped = jnp.dot(deviation, gw[g], preferred_element_type=f32)
        gain = gain_ref[:, pl.ds(pl.multiple_of(t * channels + g * lanes, lanes), lanes)]
        pooled[:, cols] = (grouped * gain).astype(bf16)
    for c in load_b:
        c.wait()

    m_p = []
    for i, q in enumerate((diagonal, near)):
        ps_m[i] = jnp.dot(pooled[...], wb[q], preferred_element_type=f32).astype(bf16)
        c = remote(ps_m.at[i], pr_m.at[i], m_send.at[i], m_recv.at[i], {"tp": near})
        c.start()
        m_p.append(c)
    for i, q in enumerate((across, t)):
        keep_m[i] = jnp.dot(pooled[...], wb[q], preferred_element_type=f32)

    d_x = [
        remote(xg.at[t, k], xg.at[t, k], d_send.at[k - 1, 1], d_recv.at[k - 1, 1], {"tp": across})
        for k in (1, 2, 3)
    ]
    d_p = [
        remote(xg.at[t, k], xg.at[t, k], d_send.at[k - 1, 2], d_recv.at[k - 1, 2], {"tp": near})
        for k in (1, 2, 3)
    ]
    d_q = [
        remote(xg.at[across, k], xg.at[across, k], d_send.at[k - 1, 3], d_recv.at[k - 1, 3], {"tp": near})
        for k in (1, 2, 3)
    ]

    def from_z(k):
        d_z[k - 1].wait_recv()
        d_x[k - 1].start()
        d_p[k - 1].start()

    def from_x(k):
        d_x[k - 1].wait_recv()
        d_q[k - 1].start()

    def from_near(k):
        d_p[k - 1].wait_recv()
        d_q[k - 1].wait_recv()

    def expand(h):
        def tile(n, carry):
            total = None
            for q in range(4):
                part = jnp.dot(
                    xg[q, 2 * h : 2 * h + 2].reshape(2 * cap, quarter),
                    wgu[n, q * quarter : (q + 1) * quarter, :],
                    preferred_element_type=f32,
                )
                total = part if total is None else total + part
            gu[n] = total
            return carry

        lax.fori_loop(0, hid_tiles, tile, 0)
        for i in range(hid_tiles):
            k = hid_tiles + i
            gate = gu[i // 2, :, (i % 2) * lanes : (i % 2 + 1) * lanes]
            up = gu[k // 2, :, (k % 2) * lanes : (k % 2 + 1) * lanes]
            hid[h, :, i * lanes : (i + 1) * lanes] = (gate / (1.0 + jnp.exp(-gate)) * up).astype(bf16)

    r_p = [
        [
            remote(ps.at[i, k], pr.at[i, k], r_send.at[i, k], r_recv.at[i, k], {"tp": near})
            for k in range(4)
        ]
        for i in range(2)
    ]
    r_x = [
        remote(xs.at[k], xr.at[k], r_send.at[2, k], r_recv.at[2, k], {"tp": across}) for k in range(4)
    ]
    r_z = [
        remote(zs.at[k], zr.at[k], z_send.at[k], z_recv.at[k], {"ep": peers[k]}) for k in range(4)
    ]

    def project(h):
        for i, q in enumerate((diagonal, across, near, t)):
            part = jnp.dot(hid[h], wd[q], preferred_element_type=f32)
            for b in range(2):
                k = 2 * h + b
                piece = part[b * cap : (b + 1) * cap]
                if i % 2 == 0:
                    ps[i // 2, k] = piece.astype(bf16)
                    r_p[i // 2][k].start()
                else:
                    keep[i // 2, k] = piece

    def send_x(k):
        r_p[0][k].wait_recv()
        xs[k] = (keep[0, k] + pr[0, k].astype(f32)).astype(bf16)
        r_x[k].start()

    def send_z(k):
        r_p[1][k].wait_recv()
        r_x[k].wait_recv()
        zs[k] = (keep[1, k] + pr[1, k].astype(f32) + xr[k].astype(f32)).astype(bf16)
        if k > 0:
            r_z[k].start()

    from_z(1)
    from_z(2)
    from_x(1)
    for c in loads:
        c.wait()
    from_near(1)
    expand(0)
    from_x(2)
    from_z(3)
    m_p[0].wait_recv()
    xs_m[...] = (keep_m[0] + pr_m[0].astype(f32)).astype(bf16)
    m_x = remote(xs_m, xr_m, m_send.at[2], m_recv.at[2], {"tp": across})
    from_x(3)
    m_x.start()
    from_near(2)
    from_near(3)
    expand(1)
    for c in load_d:
        c.wait()
    project(1)
    send_x(2)
    send_x(3)
    project(0)
    send_x(1)
    send_x(0)
    send_z(2)
    send_z(3)
    send_z(1)
    m_p[1].wait_recv()
    m_x.wait_recv()
    mix_out[...] = (keep_m[1] + pr_m[1].astype(f32) + xr_m[...].astype(f32)).astype(bf16)
    send_z(0)

    result = jnp.zeros((tokens, quarter), f32)
    for k in (0, 1, 2, 3):
        if k > 0:
            r_z[k].wait_recv()
        block = zs[0] if k == 0 else zr[k]
        result = result + shares[k] * jnp.dot(places[k], block, preferred_element_type=f32)
    exp_out[...] = result.astype(bf16)

    @pl.when(z < 3)
    def _():
        halo_copy.wait_send()

    for c in d_z + d_x + d_p + d_q + r_p[0] + r_p[1] + r_x + r_z[1:] + m_p + [m_x]:
        c.wait_send()


def fused(
    mix_input,
    group_weight,
    pool_gain,
    branch_weight,
    exp_input,
    norm_gain,
    routes,
    route_weights,
    gate_weight,
    up_weight,
    down_weight,
):
    tokens, width = exp_input.shape
    rows_mix, channels = mix_input.shape
    hidden = gate_weight.shape[2]
    quarter = width // 4
    cap = 3 * tokens // 4
    hid_tiles = hidden // lanes
    vmem = pl.BlockSpec(memory_space=pltpu.VMEM)
    anywhere = pl.BlockSpec(memory_space=pl.ANY)
    dma = pltpu.SemaphoreType.DMA
    return pl.pallas_call(
        fused_kernel,
        out_shape=(
            jax.ShapeDtypeStruct((rows_mix, quarter), bf16),
            jax.ShapeDtypeStruct((tokens, quarter), bf16),
        ),
        in_specs=[vmem] * 6 + [anywhere] * 5,
        out_specs=(vmem, vmem),
        scratch_shapes=[
            pltpu.VMEM((hid_tiles, width, 2 * lanes), bf16),
            pltpu.VMEM((4, hidden, quarter), bf16),
            pltpu.VMEM((4, channels, quarter), bf16),
            pltpu.VMEM((channels // lanes, lanes, lanes), bf16),
            pltpu.VMEM((4, tokens, quarter), bf16),
            pltpu.VMEM((4, cap, quarter), bf16),
            pltpu.VMEM((4, 4, cap, quarter), bf16),
            pltpu.VMEM((hid_tiles, 2 * cap, 2 * lanes), f32),
            pltpu.VMEM((2, 2 * cap, hidden), bf16),
            pltpu.VMEM((16, channels), bf16),
            pltpu.VMEM((rows_mix, channels), bf16),
            pltpu.VMEM((2, rows_mix, quarter), f32),
            pltpu.VMEM((2, rows_mix, quarter), bf16),
            pltpu.VMEM((2, rows_mix, quarter), bf16),
            pltpu.VMEM((rows_mix, quarter), bf16),
            pltpu.VMEM((rows_mix, quarter), bf16),
            pltpu.VMEM((2, 4, cap, quarter), f32),
            pltpu.VMEM((2, 4, cap, quarter), bf16),
            pltpu.VMEM((2, 4, cap, quarter), bf16),
            pltpu.VMEM((4, cap, quarter), bf16),
            pltpu.VMEM((4, cap, quarter), bf16),
            pltpu.VMEM((4, cap, quarter), bf16),
            pltpu.VMEM((4, cap, quarter), bf16),
            dma((2 * hid_tiles + 9,)),
            dma((3, 4)),
            dma((3, 4)),
            dma((3, 4)),
            dma((3, 4)),
            dma((4,)),
            dma((4,)),
            dma((3,)),
            dma((3,)),
            dma((2,)),
        ],
        compiler_params=pltpu.CompilerParams(
            collective_id=0, has_side_effects=True, vmem_limit_bytes=56 << 20
        ),
    )(
        exp_input,
        norm_gain.reshape(1, -1),
        routes,
        route_weights,
        mix_input,
        pool_gain.reshape(1, -1),
        group_weight,
        branch_weight,
        gate_weight,
        up_weight,
        down_weight,
    )


def fits(mesh, args):
    mix, group, _, _, tok, _, routes, _, gate, _, _ = args
    ep, tp, grp = (mesh.shape[k] for k in ("ep", "tp", "grp"))
    if ep != 4 or tp != 4 or routes.shape[1] != 2 or gate.shape[0] != ep:
        return False
    rows, channels = mix.shape[0] // (grp * ep), mix.shape[1] // tp
    tokens, quarter = tok.shape[0] // (grp * ep), tok.shape[1] // tp
    return (
        group.shape[1] == lanes
        and channels % (4 * lanes) == 0
        and channels == quarter
        and rows % 16 == 0
        and tokens % 64 == 0
        and gate.shape[2] % (tp * lanes) == 0
        and gate.shape[1] * gate.shape[2] <= 1 << 23
        and rows <= 512
        and tokens <= 256
    )


def solution(mesh):
    def run(*args):
        body = fused if fits(mesh, args) else on_device
        return jax.shard_map(
            body,
            mesh=mesh,
            in_specs=(
                P(("grp", "ep"), "tp"),
                P(),
                P(),
                P("tp", None),
                P(("grp", "ep"), None),
                P(),
                P(("grp", "ep"), None),
                P(("grp", "ep"), None),
                P("ep", None, "tp"),
                P("ep", None, "tp"),
                P("ep", "tp", None),
            ),
            out_specs=(P(("grp", "ep"), "tp"), P(("grp", "ep"), "tp")),
            check_vma=False,
        )(*args)

    return run
```

```python
import functools

import jax
import jax.numpy as jnp
from jax import lax
from jax.experimental import pallas as pl
from jax.experimental.pallas import tpu as pltpu
from jax.sharding import PartitionSpec as P

windows = (2, 4, 8, 16)
epsilon = 1e-06


def shifted(block, axis, distance):
    devices = range(lax.axis_size(axis))
    route = [(i - distance, i) for i in devices if i - distance in devices]
    return lax.ppermute(block, axis, route)


def trailing_sums(extended, rows):
    span_two = extended[1:] + extended[:-1]
    span_four = span_two[2:] + span_two[:-2]
    span_eight = span_four[4:] + span_four[:-4]
    span_sixteen = span_eight[8:] + span_eight[:-8]
    return [span_two[-rows:], span_four[-rows:], span_eight[-rows:], span_sixteen]


def pooled_deviation(extended, positions, group_ids, group_width, rows):
    sums = trailing_sums(extended, rows)
    current = extended[-rows:]
    window_id = jnp.repeat(group_ids % 4, group_width)
    result = jnp.zeros_like(current)
    for window_level, window_len in enumerate(windows):
        counted = jnp.minimum(positions + 1, window_len).astype(jnp.float32)[:, None]
        result = jnp.where(
            window_id[None, :] == window_level, sums[window_level] / counted - current, result
        )
    return result


def on_device(
    mix_input,
    group_weight,
    pool_gain,
    branch_weight,
    exp_input,
    norm_gain,
    routes,
    route_weights,
    gate_weight,
    up_weight,
    down_weight,
):
    tp_rank = lax.axis_index("tp")
    ep_rank = lax.axis_index("ep")
    rows_mix, channels = mix_input.shape
    group_width = group_weight.shape[1]
    group_count = channels // group_width
    first_group = tp_rank * group_count
    last_rows = mix_input[rows_mix - 15 :]
    before = shifted(last_rows, "ep", 1)
    extended = jnp.concatenate([before, mix_input], axis=0).astype(jnp.float32)
    positions = ep_rank * rows_mix + jnp.arange(rows_mix, dtype=jnp.int32)
    group_ids = first_group + jnp.arange(group_count, dtype=jnp.int32)
    deviation = pooled_deviation(extended, positions, group_ids, group_width, rows_mix).astype(
        jnp.bfloat16
    )
    own_groups = lax.dynamic_slice_in_dim(group_weight, first_group, group_count, 0)
    grouped = jnp.einsum(
        "rgc,gcd->rgd",
        deviation.reshape(rows_mix, group_count, group_width),
        own_groups,
        preferred_element_type=jnp.float32,
    ).reshape(rows_mix, channels)
    own_gain = lax.dynamic_slice_in_dim(pool_gain, first_group * group_width, channels, 0)
    pooled = (grouped * own_gain).astype(jnp.bfloat16)
    tok_rows, width = exp_input.shape
    columns = width // lax.axis_size("tp")
    experts_all = lax.axis_size("ep")
    capacity = 3 * tok_rows // experts_all
    floated = exp_input.astype(jnp.float32)
    normed = (
        floated
        * lax.rsqrt(jnp.mean(floated * floated, axis=1, keepdims=True) + epsilon)
        * norm_gain
    ).astype(jnp.bfloat16)
    flat_expert = routes.reshape(-1)
    assignments = flat_expert.shape[0]
    onehot = (flat_expert[:, None] == jnp.arange(experts_all, dtype=jnp.int32)[None, :]).astype(
        jnp.int32
    )
    slot_rank = jnp.sum((jnp.cumsum(onehot, axis=0) - onehot) * onehot, axis=1)
    slot_index = flat_expert * capacity + slot_rank
    token_of = jnp.arange(assignments, dtype=jnp.int32) // routes.shape[1]
    slot_token = (
        jnp.full((experts_all * capacity,), tok_rows, jnp.int32).at[slot_index].set(token_of)
    )
    padded = jnp.concatenate([normed, jnp.zeros((1, width), jnp.bfloat16)], axis=0)
    w_gate = gate_weight[0]
    w_up = up_weight[0]
    w_down = down_weight[0]
    arrived_rows = experts_all * capacity
    own_columns = lax.dynamic_slice_in_dim(padded, tp_rank * columns, columns, 1)
    outgoing = own_columns[slot_token].reshape(experts_all, capacity, columns)
    arrived = lax.all_to_all(outgoing, "ep", split_axis=0, concat_axis=0, tiled=True).reshape(
        arrived_rows, columns
    )
    section = lax.all_gather(arrived, "tp", axis=1, tiled=True)
    gate_pre = jnp.dot(section, w_gate, preferred_element_type=jnp.float32)
    up_pre = jnp.dot(section, w_up, preferred_element_type=jnp.float32)
    hidden = (jax.nn.silu(gate_pre) * up_pre).astype(jnp.bfloat16)
    weight_cols = branch_weight
    mix_sum = lax.psum_scatter(
        lax.dot_general(
            weight_cols, pooled, (((0,), (1,)), ((), ())), preferred_element_type=jnp.float32
        ).astype(jnp.bfloat16),
        "tp",
        scatter_dimension=0,
        tiled=True,
    )
    weight_cols = w_down
    exp_sum = lax.psum_scatter(
        lax.dot_general(
            weight_cols, hidden, (((0,), (1,)), ((), ())), preferred_element_type=jnp.float32
        ).astype(jnp.bfloat16),
        "tp",
        scatter_dimension=0,
        tiled=True,
    )
    mix_out = mix_sum.T
    results = exp_sum.reshape(columns, experts_all, capacity)
    returned = lax.all_to_all(results, "ep", split_axis=1, concat_axis=1, tiled=True).reshape(
        columns, experts_all * capacity
    )
    picked = returned[:, slot_index].astype(jnp.float32)
    weighted = picked * route_weights.reshape(-1)[None, :]
    combined = jnp.sum(weighted.reshape(columns, tok_rows, routes.shape[1]), axis=2)
    exp_out = combined.T.astype(jnp.bfloat16)
    return (mix_out, exp_out)


lanes = 128
MESH = pl.DeviceIdType.MESH
f32 = jnp.float32
bf16 = jnp.bfloat16


def fused_kernel(
    x_ref,
    norm_ref,
    routes_ref,
    weights_ref,
    mix_ref,
    gain_ref,
    groups_hbm,
    branch_hbm,
    gate_hbm,
    up_hbm,
    down_hbm,
    mix_out,
    exp_out,
    wgu,
    wd,
    wb,
    gw,
    xn,
    sb,
    xg,
    gu,
    hid,
    halo,
    pooled,
    keep_m,
    ps_m,
    pr_m,
    xs_m,
    xr_m,
    keep,
    ps,
    pr,
    xs,
    xr,
    zs,
    zr,
    w_sem,
    d_send,
    d_recv,
    r_send,
    r_recv,
    z_send,
    z_recv,
    m_send,
    m_recv,
    h_sem,
):
    z = lax.axis_index("ep")
    t = lax.axis_index("tp")
    near = t + 1 - 2 * (t % 2)
    across = (t + 2) % 4
    diagonal = (near + 2) % 4
    peers = [z, z + 1 - 2 * (z % 2), 3 - z, (z + 2) % 4]
    tokens, width = x_ref.shape
    quarter = width // 4
    cap = xg.shape[2]
    hid_tiles = gate_hbm.shape[2] // lanes
    rows_mix, channels = mix_ref.shape
    group_count = channels // lanes

    loads = []
    for i in range(2 * hid_tiles):
        src = gate_hbm if i < hid_tiles else up_hbm
        at = (i % hid_tiles) * lanes
        loads.append(
            pltpu.make_async_copy(
                src.at[0, :, pl.ds(at, lanes)],
                wgu.at[i // 2, :, pl.ds((i % 2) * lanes, lanes)],
                w_sem.at[i],
            )
        )
    n0 = 2 * hid_tiles
    load_b = [
        pltpu.make_async_copy(branch_hbm.at[:, pl.ds(k * quarter, quarter)], wb.at[k], w_sem.at[n0 + k])
        for k in range(4)
    ]
    load_d = [
        pltpu.make_async_copy(down_hbm.at[0, :, pl.ds(k * quarter, quarter)], wd.at[k], w_sem.at[n0 + 4 + k])
        for k in range(4)
    ]
    load_g = pltpu.make_async_copy(groups_hbm.at[pl.ds(t * group_count, group_count)], gw, w_sem.at[n0 + 8])
    load_g.start()
    for c in load_b + loads + load_d:
        c.start()

    barrier = pltpu.get_barrier_semaphore()
    for k in (1, 2, 3):
        pl.semaphore_signal(barrier, inc=1, device_id={"ep": peers[k]}, device_id_type=MESH)
    for k in (near, across):
        pl.semaphore_signal(barrier, inc=1, device_id={"tp": k}, device_id_type=MESH)

    def remote(src, dst, send, recv, who):
        return pltpu.make_async_remote_copy(
            src_ref=src, dst_ref=dst, send_sem=send, recv_sem=recv, device_id=who, device_id_type=MESH
        )

    floated = x_ref[...].astype(f32)
    scale = lax.rsqrt(jnp.mean(floated * floated, axis=1, keepdims=True) + epsilon)
    xn_val = (floated * scale * norm_ref[...]).astype(bf16)
    for k in range(4):
        xn[k] = xn_val[:, k * quarter : (k + 1) * quarter]
    lane = lax.broadcasted_iota(jnp.int32, (tokens, lanes), 1)
    square = (tokens, tokens)
    diagonal_mask = lax.broadcasted_iota(jnp.int32, square, 0) == lax.broadcasted_iota(jnp.int32, square, 1)

    def column(row):
        spread = jnp.broadcast_to(row, square)
        return jnp.sum(jnp.where(diagonal_mask, spread, jnp.zeros_like(spread)), axis=1, keepdims=True)

    r0 = column(routes_ref[0:1, :].astype(f32)).astype(jnp.int32)
    r1 = column(routes_ref[1:2, :].astype(f32)).astype(jnp.int32)
    w0 = column(weights_ref[0:1, :])
    w1 = column(weights_ref[1:2, :])
    member = ((r0 == lane) | (r1 == lane)).astype(f32)
    above = (
        lax.broadcasted_iota(jnp.int32, (tokens, tokens), 0)
        > lax.broadcasted_iota(jnp.int32, (tokens, tokens), 1)
    ).astype(f32)
    rank = jnp.dot(above.astype(bf16), member.astype(bf16), preferred_element_type=f32)
    slot_lane = lax.broadcasted_iota(jnp.int32, (tokens, cap), 1)
    places = []
    shares = []
    for k in range(4):
        own = jnp.sum(jnp.where(lane == peers[k], rank, 0.0), axis=1, keepdims=True).astype(jnp.int32)
        named = (r0 == peers[k]) | (r1 == peers[k])
        slot = jnp.where(named, own, cap)
        places.append((slot_lane == slot).astype(f32).astype(bf16))
        shares.append(
            jnp.where(r0 == peers[k], w0, 0.0)
            + jnp.where(r1 == peers[k], w1, 0.0)
        )

    def gathered(k, block):
        return lax.dot_general(
            places[k], block, (((0,), (0,)), ((), ())), preferred_element_type=f32
        ).astype(bf16)

    own_cols = xn[t]
    for k in (1, 2, 3):
        sb[k] = gathered(k, own_cols)
    pl.semaphore_wait(barrier, 5)
    halo_copy = remote(
        mix_ref.at[pl.ds(rows_mix - 16, 16), :], halo, h_sem.at[0], h_sem.at[1], {"ep": (z + 1) % 4}
    )

    @pl.when(z < 3)
    def _():
        halo_copy.start()

    d_z = []
    for k in (1, 2, 3):
        c = remote(sb.at[k], xg.at[t, k], d_send.at[k - 1, 0], d_recv.at[k - 1, 0], {"ep": peers[k]})
        c.start()
        d_z.append(c)
    for q in range(4):
        xg[q, 0] = gathered(0, xn[q])

    @pl.when(z == 0)
    def _():
        halo[...] = jnp.zeros_like(halo)

    @pl.when(z > 0)
    def _():
        halo_copy.wait_recv()

    load_g.wait()
    position = z * rows_mix + lax.broadcasted_iota(jnp.int32, (rows_mix, lanes), 0)
    for g in range(group_count):
        cols = slice(g * lanes, (g + 1) * lanes)
        current = mix_ref[:, cols].astype(f32)
        total = jnp.concatenate([halo[:, cols].astype(f32), current], axis=0)
        level = g % 4
        for step in range(level + 1):
            total = total + pltpu.roll(total, 1 << step, 0)
        counted = jnp.minimum(position + 1, windows[level]).astype(f32)
        deviation = (total[16:] / counted - current).astype(bf16)
        grouped = jnp.dot(deviation, gw[g], preferred_element_type=f32)
        gain = gain_ref[:, pl.ds(pl.multiple_of(t * channels + g * lanes, lanes), lanes)]
        pooled[:, cols] = (grouped * gain).astype(bf16)
    for c in load_b:
        c.wait()

    m_p = []
    for i, q in enumerate((diagonal, near)):
        ps_m[i] = jnp.dot(pooled[...], wb[q], preferred_element_type=f32).astype(bf16)
        c = remote(ps_m.at[i], pr_m.at[i], m_send.at[i], m_recv.at[i], {"tp": near})
        c.start()
        m_p.append(c)
    for i, q in enumerate((across, t)):
        keep_m[i] = jnp.dot(pooled[...], wb[q], preferred_element_type=f32)

    d_x = [
        remote(xg.at[t, k], xg.at[t, k], d_send.at[k - 1, 1], d_recv.at[k - 1, 1], {"tp": across})
        for k in (1, 2, 3)
    ]
    d_p = [
        remote(xg.at[t, k], xg.at[t, k], d_send.at[k - 1, 2], d_recv.at[k - 1, 2], {"tp": near})
        for k in (1, 2, 3)
    ]
    d_q = [
        remote(xg.at[across, k], xg.at[across, k], d_send.at[k - 1, 3], d_recv.at[k - 1, 3], {"tp": near})
        for k in (1, 2, 3)
    ]

    def from_z(k):
        d_z[k - 1].wait_recv()
        d_x[k - 1].start()
        d_p[k - 1].start()

    def from_x(k):
        d_x[k - 1].wait_recv()
        d_q[k - 1].start()

    def from_near(k):
        d_p[k - 1].wait_recv()
        d_q[k - 1].wait_recv()

    def expand(h, first, last):
        def tile(n, carry):
            total = None
            for q in range(4):
                part = jnp.dot(
                    xg[q, 2 * h : 2 * h + 2].reshape(2 * cap, quarter),
                    wgu[n, q * quarter : (q + 1) * quarter, :],
                    preferred_element_type=f32,
                )
                total = part if total is None else total + part
            gu[n] = total
            return carry

        lax.fori_loop(first, last, tile, 0)

    def activate(h):
        for i in range(hid_tiles):
            k = hid_tiles + i
            gate = gu[i // 2, :, (i % 2) * lanes : (i % 2 + 1) * lanes]
            up = gu[k // 2, :, (k % 2) * lanes : (k % 2 + 1) * lanes]
            hid[h, :, i * lanes : (i + 1) * lanes] = (gate / (1.0 + jnp.exp(-gate)) * up).astype(bf16)

    r_p = [
        [
            remote(ps.at[i, k], pr.at[i, k], r_send.at[i, k], r_recv.at[i, k], {"tp": near})
            for k in range(4)
        ]
        for i in range(2)
    ]
    r_x = [
        remote(xs.at[k], xr.at[k], r_send.at[2, k], r_recv.at[2, k], {"tp": across}) for k in range(4)
    ]
    r_z = [
        remote(zs.at[k], zr.at[k], z_send.at[k], z_recv.at[k], {"ep": peers[k]}) for k in range(4)
    ]

    def project(h):
        for i, q in enumerate((diagonal, across, near, t)):
            part = jnp.dot(hid[h], wd[q], preferred_element_type=f32)
            for b in range(2):
                k = 2 * h + b
                piece = part[b * cap : (b + 1) * cap]
                if i % 2 == 0:
                    ps[i // 2, k] = piece.astype(bf16)
                    r_p[i // 2][k].start()
                else:
                    keep[i // 2, k] = piece

    def send_x(k):
        r_p[0][k].wait_recv()
        xs[k] = (keep[0, k] + pr[0, k].astype(f32)).astype(bf16)
        r_x[k].start()

    def send_z(k):
        r_p[1][k].wait_recv()
        r_x[k].wait_recv()
        zs[k] = (keep[1, k] + pr[1, k].astype(f32) + xr[k].astype(f32)).astype(bf16)
        if k > 0:
            r_z[k].start()

    half = hid_tiles // 2
    from_z(1)
    from_z(2)
    from_x(1)
    for c in loads:
        c.wait()
    from_near(1)
    expand(0, 0, half)
    from_x(2)
    from_z(3)
    expand(0, half, hid_tiles)
    activate(0)
    for c in load_d:
        c.wait()
    project(0)
    from_x(3)
    send_x(1)
    send_x(0)
    from_near(2)
    from_near(3)
    expand(1, 0, hid_tiles)
    activate(1)
    project(1)
    send_x(2)
    send_x(3)
    m_p[0].wait_recv()
    xs_m[...] = (keep_m[0] + pr_m[0].astype(f32)).astype(bf16)
    m_x = remote(xs_m, xr_m, m_send.at[2], m_recv.at[2], {"tp": across})
    m_x.start()
    send_z(1)
    send_z(0)
    send_z(2)
    send_z(3)
    m_p[1].wait_recv()
    mix_sum = keep_m[1] + pr_m[1].astype(f32)

    def share(k):
        block = zs[0] if k == 0 else zr[k]
        return shares[k] * jnp.dot(places[k], block, preferred_element_type=f32)

    result = share(0)
    r_z[1].wait_recv()
    result = result + share(1)
    m_x.wait_recv()
    mix_out[...] = (mix_sum + xr_m[...].astype(f32)).astype(bf16)
    for k in (2, 3):
        r_z[k].wait_recv()
        result = result + share(k)
    exp_out[...] = result.astype(bf16)

    @pl.when(z < 3)
    def _():
        halo_copy.wait_send()

    for c in d_z + d_x + d_p + d_q + r_p[0] + r_p[1] + r_x + r_z[1:] + m_p + [m_x]:
        c.wait_send()


def fused(
    mix_input,
    group_weight,
    pool_gain,
    branch_weight,
    exp_input,
    norm_gain,
    routes,
    route_weights,
    gate_weight,
    up_weight,
    down_weight,
):
    tokens, width = exp_input.shape
    rows_mix, channels = mix_input.shape
    hidden = gate_weight.shape[2]
    quarter = width // 4
    cap = 3 * tokens // 4
    hid_tiles = hidden // lanes
    vmem = pl.BlockSpec(memory_space=pltpu.VMEM)
    anywhere = pl.BlockSpec(memory_space=pl.ANY)
    dma = pltpu.SemaphoreType.DMA
    return pl.pallas_call(
        fused_kernel,
        out_shape=(
            pltpu.VMEM((rows_mix, quarter), bf16),
            pltpu.VMEM((tokens, quarter), bf16),
        ),
        in_specs=[vmem] * 6 + [anywhere] * 5,
        out_specs=(vmem, vmem),
        scratch_shapes=[
            pltpu.VMEM((hid_tiles, width, 2 * lanes), bf16),
            pltpu.VMEM((4, hidden, quarter), bf16),
            pltpu.VMEM((4, channels, quarter), bf16),
            pltpu.VMEM((channels // lanes, lanes, lanes), bf16),
            pltpu.VMEM((4, tokens, quarter), bf16),
            pltpu.VMEM((4, cap, quarter), bf16),
            pltpu.VMEM((4, 4, cap, quarter), bf16),
            pltpu.VMEM((hid_tiles, 2 * cap, 2 * lanes), f32),
            pltpu.VMEM((2, 2 * cap, hidden), bf16),
            pltpu.VMEM((16, channels), bf16),
            pltpu.VMEM((rows_mix, channels), bf16),
            pltpu.VMEM((2, rows_mix, quarter), f32),
            pltpu.VMEM((2, rows_mix, quarter), bf16),
            pltpu.VMEM((2, rows_mix, quarter), bf16),
            pltpu.VMEM((rows_mix, quarter), bf16),
            pltpu.VMEM((rows_mix, quarter), bf16),
            pltpu.VMEM((2, 4, cap, quarter), f32),
            pltpu.VMEM((2, 4, cap, quarter), bf16),
            pltpu.VMEM((2, 4, cap, quarter), bf16),
            pltpu.VMEM((4, cap, quarter), bf16),
            pltpu.VMEM((4, cap, quarter), bf16),
            pltpu.VMEM((4, cap, quarter), bf16),
            pltpu.VMEM((4, cap, quarter), bf16),
            dma((2 * hid_tiles + 9,)),
            dma((3, 4)),
            dma((3, 4)),
            dma((3, 4)),
            dma((3, 4)),
            dma((4,)),
            dma((4,)),
            dma((3,)),
            dma((3,)),
            dma((2,)),
        ],
        compiler_params=pltpu.CompilerParams(
            collective_id=0, has_side_effects=True, vmem_limit_bytes=56 << 20
        ),
    )(
        exp_input,
        norm_gain.reshape(1, -1),
        routes.T,
        route_weights.T,
        mix_input,
        pool_gain.reshape(1, -1),
        group_weight,
        branch_weight,
        gate_weight,
        up_weight,
        down_weight,
    )


def fits(mesh, args):
    mix, group, _, _, tok, _, routes, _, gate, _, _ = args
    ep, tp, grp = (mesh.shape[k] for k in ("ep", "tp", "grp"))
    if ep != 4 or tp != 4 or routes.shape[1] != 2 or gate.shape[0] != ep:
        return False
    rows, channels = mix.shape[0] // (grp * ep), mix.shape[1] // tp
    tokens, quarter = tok.shape[0] // (grp * ep), tok.shape[1] // tp
    return (
        group.shape[1] == lanes
        and channels % (4 * lanes) == 0
        and channels == quarter
        and rows % 16 == 0
        and tokens % 64 == 0
        and gate.shape[2] % (tp * lanes) == 0
        and gate.shape[1] * gate.shape[2] <= 1 << 23
        and rows <= 512
        and tokens <= 256
    )


def solution(mesh):
    def run(*args):
        body = fused if fits(mesh, args) else on_device
        return jax.shard_map(
            body,
            mesh=mesh,
            in_specs=(
                P(("grp", "ep"), "tp"),
                P(),
                P(),
                P("tp", None),
                P(("grp", "ep"), None),
                P(),
                P(("grp", "ep"), None),
                P(("grp", "ep"), None),
                P("ep", None, "tp"),
                P("ep", None, "tp"),
                P("ep", "tp", None),
            ),
            out_specs=(P(("grp", "ep"), "tp"), P(("grp", "ep"), "tp")),
            check_vma=False,
        )(*args)

    return run
```
